32 devices in a mesh: sp: 8 (over z, y), tp: 4 (over x, core).
Axes of the slice: x: 2, y: 2, z: 4, core: 2. Of those that a mesh axis runs over, the one named last changes fastest.
Arguments:
- queries: bfloat16 [1536, 2048], P('sp', 'tp'), may hold values from -100 to 100
- keys: bfloat16 [1536, 512], P('sp'), may hold values from -8 to 8
- values: bfloat16 [1536, 512], P('sp'), may hold values from -6 to 6
- diff_scale: float32 [8], P('tp'), may hold values from 0.3 to 0.8
- head_gain: float32 [256], replicated, may hold values from 0.1 to 1.9
- w_out: bfloat16 [2048, 2048], P('tp'), may hold values from -0.125 to 0.125
- residual: bfloat16 [1536, 2048], P(('sp', 'tp')), may hold values from -6 to 6
- norm_gain: float32 [2048], replicated, may hold values from 0.1 to 1.9
- route_ids: int32 [1536, 2], P(('sp', 'tp')), may hold values from 0 to 7, all different within a row; in each aligned block of 48 rows (0 to 47, 48 to 95, ...) at most 18 rows name the same one
- route_weights: float32 [1536, 2], P(('sp', 'tp')), may hold values from 0.2 to 1
- w_gate: bfloat16 [8, 2048, 3072], P('sp', None, 'tp'), may hold values from -0.125 to 0.125
- w_up: bfloat16 [8, 2048, 3072], P('sp', None, 'tp'), may hold values from -0.125 to 0.125
- w_down: bfloat16 [8, 3072, 2048], P('sp', 'tp'), may hold values from -0.109375 to 0.109375
Outputs:
- layer_out: bfloat16 [1536, 2048], P(('sp', 'tp'))
The draws below stay inside these ranges and needn't reach their ends.
Inputs may be any that keep to these rules, and one draw needn't show every extreme that they name: `route_ids`: in each aligned block of 48 rows (the rows of one device), no expert is named more than 18 times, a bound that some block reaches; a row names 2 different experts.
All inputs are finite; a program needn't handle non-finite values.
Results may differ from the reference program's by a relative error of at most 0.014.
Values may be sent and summed in bfloat16 or wider, within the bound.
A program may use at most 128 MiB of HBM per device.

```python
import math
import jax
import jax.numpy as jnp
import numpy as np
from jax import lax

HEAD_DIM = 128
V_DIM = 256
HEADS = 8
KV_HEADS = 2
D = 2048
FF = 3072
TOP = 2
TOKENS = 1536
ROWS = 48
FF_DEV = 768
EXPERTS = 8
CAP = 18
N_TP = 4


def paired(key):
    base = jax.random.fold_in(key, 11)
    key_q, key_k = jax.random.split(base, 2)
    queries = jnp.clip(jax.random.normal(key_q, (TOKENS, HEADS * 2 * HEAD_DIM), jnp.float32) * 1.3, -8.0, 8.0)
    keys = jnp.clip(jax.random.normal(key_k, (TOKENS, KV_HEADS * 2 * HEAD_DIM), jnp.float32) * 1.3, -8.0, 8.0)
    return (queries, keys)


def draw_queries(key, part):
    return paired(key)[0].astype(jnp.bfloat16)


def draw_keys(key, part):
    return paired(key)[1].astype(jnp.bfloat16)


def block_levels(key, shape, shards, low, largest):
    factor_of, own = 1.0, jax.random.fold_in(key, 6)
    for dim, blocks in shards:
        steps = jnp.exp(jax.random.uniform(jax.random.fold_in(own, dim), (blocks,), jnp.float32, low / len(shards), largest / len(shards)))
        factor_of = factor_of * jnp.repeat(steps, shape[dim] // blocks).reshape([-1 if axis == dim else 1 for axis in range(len(shape))])
    return factor_of


def assign_block(own_key, own, number, rows, amount, top, bound, slope):
    sequence = jax.random.permutation(own_key, amount)
    packed, ordinary = shares(amount, rows * top, bound, slope, True), shares(amount, rows * top, bound, slope, False)
    places = jnp.arange(amount)

    def named(tallies, turn):
        used = int((tallies > 0).sum())
        fixed = max(1, used // 4)
        passed = fixed + (places - fixed + turn * (used - fixed)) % max(1, amount - fixed)
        return jnp.zeros((amount,), jnp.int32).at[sequence[jnp.where(places < fixed, places, passed)]].set(jnp.asarray(tallies, jnp.int32))

    tallies = jnp.where(number % 4 == 0, named(packed, number // 4), named(ordinary, number - number // 4 - 1))
    mixed = jax.random.permutation(jax.random.fold_in(own, 3), amount)
    donor, taker = mixed[0:amount // 2 * 2:2], mixed[1:amount // 2 * 2:2]
    slack = jnp.minimum(tallies[donor] - 1, bound - tallies[taker]) // 2
    slack = jnp.where((donor == sequence[0]) | (taker == sequence[0]) | (tallies[taker] == 0), 0, jnp.maximum(slack, 0))
    passed = jax.random.randint(jax.random.fold_in(own, 4), (amount // 2,), 0, 1 << 20) % (slack + 1)
    tallies = tallies.at[donor].add(-passed).at[taker].add(passed)
    labels = jnp.searchsorted(jnp.cumsum(tallies), jnp.arange(rows * top), side="right").astype(jnp.int32)
    table = labels.reshape(top, rows).T
    table = table[jax.random.permutation(jax.random.fold_in(own, 1), rows)]
    turn = jax.random.randint(jax.random.fold_in(own, 2), (rows, 1), 0, top)
    return jnp.take_along_axis(table, (jnp.arange(top)[None, :] + turn) % top, axis=1)


def shares(amount, total, limit, skew, full):
    portions = [(1 << 20) // math.isqrt(rank ** skew) + 1 for rank in range(1, amount + 1)]
    largest = limit if full else min(limit, max(-(-total // amount), total * portions[0] // sum(portions)))
    least = 1 if total - largest >= amount - 1 else 0
    counts, rest = [largest] + [least] * (amount - 1), total - largest - least * (amount - 1)
    while rest > 0:
        movable = [i for i in range(1, amount) if counts[i] < largest] or [i for i in range(1, amount) if counts[i] < limit]
        pool, left = sum([portions[i] for i in movable]), rest
        for i in movable:
            addition = min(limit - counts[i], max(1, left * portions[i] // pool), rest)
            counts[i] = counts[i] + addition
            rest = rest - addition
    return np.array(counts)


def centred(own_key, shape, width, bound, pieces=(), held_as=jnp.bfloat16):
    drawn = jax.random.normal(own_key, shape, jnp.float32) * width
    if len(pieces) > 0:
        drawn = block_levels(own_key, shape, pieces, -0.22, 0.18) * drawn
    return jnp.clip(drawn, min=-bound, max=bound).astype(held_as)


def setup_inputs(seed: int = 0) -> dict:
    key_of = jax.random.split(jax.random.key(seed), 14)
    queries = draw_queries(jax.random.fold_in(key_of[13], 71), 0)
    keys = draw_keys(jax.random.fold_in(key_of[13], 71), 0)
    values = centred(key_of[2], (TOKENS, KV_HEADS * V_DIM), 1.0, 6.0, ((0, 8),))
    diff_scale = jnp.clip(0.3 + 0.5 * jax.random.uniform(key_of[3], (HEADS,), jnp.float32) ** block_levels(key_of[3], (HEADS,), ((0, 4),), -0.2, 0.2), 0.3, 0.8)
    head_gain = jnp.clip(1.0 + 0.18 * jax.random.normal(key_of[4], (V_DIM,), jnp.float32), 0.1, 1.9)
    w_out = centred(key_of[5], (HEADS * V_DIM, D), (HEADS * V_DIM) ** -0.5, 0.125, ((0, 4),))
    residual = centred(key_of[6], (TOKENS, D), 1.0, 6.0, ((0, 32),))
    norm_gain = jnp.clip(1.0 + 0.18 * jax.random.normal(key_of[7], (D,), jnp.float32), 0.1, 1.9)
    route_ids_keys = jax.random.split(jax.random.fold_in(key_of[8], 1), TOKENS // ROWS)
    route_ids_turns = jax.random.permutation(jax.random.fold_in(key_of[8], 3), TOKENS // ROWS)
    route_ids = jax.vmap(lambda own, number: assign_block(jax.random.fold_in(key_of[8], 2), own, number, ROWS, EXPERTS, TOP, CAP, 1))(route_ids_keys, route_ids_turns).reshape((TOKENS, TOP))
    route_weights = jnp.clip(0.2 + 0.8 * jax.random.uniform(key_of[9], (TOKENS, TOP), jnp.float32) ** block_levels(key_of[9], (TOKENS, TOP), ((0, 32),), -0.2, 0.2), 0.2, 1.0)
    w_gate = centred(key_of[10], (EXPERTS, D, FF), D ** -0.5, 0.125, ((0, 8), (2, 4)))
    w_up = centred(key_of[11], (EXPERTS, D, FF), D ** -0.5, 0.125, ((0, 8), (2, 4)))
    w_down = centred(key_of[12], (EXPERTS, FF, D), FF ** -0.5, 0.109375, ((0, 8), (1, 4)))
    return {"queries": queries, "keys": keys, "values": values, "diff_scale": diff_scale, "head_gain": head_gain, "w_out": w_out, "residual": residual, "norm_gain": norm_gain, "route_ids": route_ids, "route_weights": route_weights, "w_gate": w_gate, "w_up": w_up, "w_down": w_down}


EPS = 1e-06

def rounded(value):
    return lax.optimization_barrier(value.astype(jnp.bfloat16)).astype(jnp.float32)

def reference(queries, keys, values, diff_scale, head_gain, w_out, residual, norm_gain, route_ids, route_weights, w_gate, w_up, w_down):
    q_heads = queries.reshape(TOKENS, HEADS, 2, HEAD_DIM)
    k_groups = keys.reshape(TOKENS, KV_HEADS, 2, HEAD_DIM).astype(jnp.float32)
    v_groups = values.reshape(TOKENS, KV_HEADS, V_DIM).astype(jnp.float32)
    block = math.gcd(TOKENS, 512)
    per_group = HEADS // KV_HEADS

    def attend_block(q_block):
        outs = []
        for head in range(HEADS):
            grp = head // per_group
            scores = jnp.einsum('qmd,kmd->mqk', q_block[:, head].astype(jnp.float32), k_groups[:, grp]) / math.sqrt(HEAD_DIM)
            peak = lax.optimization_barrier(jnp.max(scores, axis=-1, keepdims=True))
            weights = rounded(jnp.exp(scores - peak))
            totals = lax.optimization_barrier(jnp.sum(weights, axis=-1))
            numer = jnp.einsum('mqk,kd->mqd', weights, v_groups[:, grp])
            outs.append(numer[0] / totals[0][:, None] - diff_scale[head] * numer[1] / totals[1][:, None])
        mixed = jnp.stack(outs, axis=1)
        normal_part = mixed * lax.rsqrt(lax.optimization_barrier(jnp.mean(mixed * mixed, axis=-1, keepdims=True)) + EPS) * head_gain
        return normal_part.astype(jnp.bfloat16).reshape(block, HEADS * V_DIM)
    head_out = lax.map(attend_block, q_heads.reshape(TOKENS // block, block, HEADS, 2, HEAD_DIM)).reshape(TOKENS, HEADS * V_DIM)
    width_dev = HEADS * V_DIM // N_TP
    attended = jnp.zeros((TOKENS, D), jnp.float32)
    for part in range(N_TP):
        attended = attended + rounded(jnp.dot(head_out[:, part * width_dev:(part + 1) * width_dev], w_out[part * width_dev:(part + 1) * width_dev], preferred_element_type=jnp.float32))
    state = residual.astype(jnp.float32) + attended
    normed = (state * lax.rsqrt(lax.optimization_barrier(jnp.mean(state * state, axis=-1, keepdims=True)) + EPS) * norm_gain).astype(jnp.bfloat16)
    blocks = TOKENS // ROWS
    ids = route_ids.reshape(blocks, ROWS * TOP)
    onehot = (ids[:, :, None] == jnp.arange(EXPERTS, dtype=jnp.int32)[None, None, :]).astype(jnp.int32)
    slot = lax.optimization_barrier(jnp.sum((jnp.cumsum(onehot, axis=1) - onehot) * onehot, axis=-1))
    dest = (ids * (blocks * CAP) + jnp.arange(blocks, dtype=jnp.int32)[:, None] * CAP + slot).reshape(-1).astype(jnp.int32)
    copies = jnp.repeat(normed, TOP, axis=0)
    buffer = jnp.zeros((EXPERTS * blocks * CAP, D), jnp.bfloat16).at[dest].set(copies).reshape(EXPERTS, blocks * CAP, D)

    def serve(inputs):
        rows_in, gate_w, up_w, down_w = inputs
        gate = jnp.dot(rows_in, gate_w, preferred_element_type=jnp.float32)
        up = jnp.dot(rows_in, up_w, preferred_element_type=jnp.float32)
        hidden = (jax.nn.silu(gate) * up).astype(jnp.bfloat16)
        summed = jnp.zeros((rows_in.shape[0], D), jnp.float32)
        for part in range(N_TP):
            summed = summed + rounded(jnp.dot(hidden[:, part * FF_DEV:(part + 1) * FF_DEV], down_w[part * FF_DEV:(part + 1) * FF_DEV], preferred_element_type=jnp.float32))
        return summed.astype(jnp.bfloat16)
    served = lax.map(serve, (buffer, w_gate, w_up, w_down)).reshape(-1, D)
    picked = served[dest].reshape(TOKENS, TOP, D)
    expert_sum = jnp.einsum('rt,rtd->rd', route_weights.astype(jnp.float32), picked.astype(jnp.float32))
    return (state + expert_sum).astype(jnp.bfloat16)
```

```python
import functools
import math

import jax
import jax.numpy as jnp
from jax import lax
from jax.experimental import pallas as pl
from jax.experimental.pallas import tpu as pltpu
from jax.sharding import PartitionSpec as P

KV_HEADS = 2
EPS = 1e-06
LOWEST = -1e30
MESH = pl.DeviceIdType.MESH
F32 = jnp.float32
BF16 = jnp.bfloat16
SUB = 16


def dot(a, b):
    return jnp.dot(a, b, preferred_element_type=F32)


def dot_t(a, b):
    return lax.dot_general(a, b, (((0,), (0,)), ((), ())), preferred_element_type=F32)


def iota(shape, dim):
    return lax.broadcasted_iota(jnp.int32, shape, dim)


def kernel(
    n_sp, n_tp, main, rest,
    q_ref, k_ref, v_ref, scale_ref, hgain_ref, wout_hbm, resid_ref, ngain_ref, ids_ref, rw_ref,
    wg_hbm, wu_hbm, wd_hbm,
    out_ref,
    wout, wg, wu, wd, kv, qs, high, total, acc, heads, proj, ra, sb, rb, state,
    om, ol, xm, xl, ym, yl, prm, prl, xsm, xsl, xrm, xrl, rsm, rsl, rtm, rtl, xin, hid, ytail,
    w_sem, kv_s, kv_r, kf_s, kf_r, ra_s, ra_r, rb_s, rb_r,
    a_s, a_r, pf_s, pf_r, xf_s, xf_r, rl_s, rl_r, pr_s, pr_r, xs_s, xs_r, rt_s, rt_r,
):
    me = lax.axis_index("sp")
    tp = lax.axis_index("tp")
    side = lax.rem(tp, 2)
    pair = tp // 2
    o_pair = 1 - pair
    o_side = 1 - side
    partner = tp + 1 - 2 * side
    across = lax.rem(tp + 2, n_tp)

    def peer_to(d):
        return lax.rem(me + d, n_sp)

    def peer_from(d):
        return lax.rem(me + n_sp - d, n_sp)

    def copy(src, dst, send, recv, sp, t):
        return pltpu.make_async_remote_copy(
            src_ref=src, dst_ref=dst, send_sem=send, recv_sem=recv, device_id=(sp, t), device_id_type=MESH
        )

    def loop(low, top, body):
        def step(i, carry):
            body(i)
            return carry

        lax.fori_loop(low, top, step, 0)

    loads = [
        pltpu.make_async_copy(wout_hbm, wout, w_sem.at[0]),
        pltpu.make_async_copy(wg_hbm.at[0], wg, w_sem.at[1]),
        pltpu.make_async_copy(wu_hbm.at[0], wu, w_sem.at[2]),
        pltpu.make_async_copy(wd_hbm.at[0], wd, w_sem.at[3]),
    ]

    barrier = pltpu.get_barrier_semaphore()
    loop(1, n_sp, lambda d: pl.semaphore_signal(barrier, inc=1, device_id=(peer_to(d), tp), device_id_type=MESH))
    for other in (1, 2, 3):
        pl.semaphore_signal(
            barrier, inc=1, device_id=(me, lax.rem(tp + other, n_tp)), device_id_type=MESH
        )

    rows = q_ref.shape[0]
    half_rows = rows // 2
    k_cols = k_ref.shape[1] // KV_HEADS
    v_cols = v_ref.shape[1] // KV_HEADS
    half = k_cols // 2
    group = tp // (n_tp // KV_HEADS)
    kv[me, :, :k_cols] = k_ref[:, pl.ds(pl.multiple_of(group * k_cols, 128), k_cols)]
    kv[me, :, k_cols:] = v_ref[:, pl.ds(pl.multiple_of(group * v_cols, 128), v_cols)]
    n_head = q_ref.shape[1] // (2 * half)
    for m in range(2):
        for h in range(n_head):
            qs[m, h * rows : (h + 1) * rows, :] = q_ref[:, (h * 2 + m) * half : (h * 2 + m + 1) * half]
    high[...] = jnp.full(high.shape, LOWEST, F32)
    total[...] = jnp.zeros(total.shape, F32)
    acc[...] = jnp.zeros(acc.shape, F32)
    pl.semaphore_wait(barrier, n_sp - 1 + 3)

    mine = pl.ds(pl.multiple_of(side * half_rows, SUB), half_rows)
    theirs = pl.ds(pl.multiple_of(o_side * half_rows, SUB), half_rows)

    def kv_send(d):
        p = peer_to(d)
        return copy(kv.at[me, mine], kv.at[me, mine], kv_s.at[p], kv_r.at[me], p, tp)

    def kv_wait(p):
        copy(kv.at[p, mine], kv.at[p, mine], kv_s.at[p], kv_r.at[p], p, tp).wait_recv()

    def kv_forward(p):
        return copy(kv.at[p, mine], kv.at[p, mine], kf_s.at[p], kf_r.at[p], me, partner)

    def far_wait(p):
        copy(kv.at[p, theirs], kv.at[p, theirs], kf_s.at[p], kf_r.at[p], me, partner).wait_recv()

    loop(1, n_sp, lambda d: kv_send(d).start())
    for load in loads:
        load.start()

    factor = 1.0 / math.sqrt(half)

    def attend(p):
        v_block = kv[p, :, k_cols:]
        for m in range(2):
            k_block = kv[p, :, m * half : (m + 1) * half]
            scores = lax.dot_general(
                qs[m], k_block, (((1,), (1,)), ((), ())), preferred_element_type=F32
            ) * factor
            old = high[m]
            peak = jnp.maximum(old, jnp.max(scores, axis=-1, keepdims=True))
            fade = jnp.exp(old - peak)
            weights = jnp.exp(scores - peak).astype(BF16)
            total[m] = total[m] * fade + jnp.sum(weights.astype(F32), axis=-1, keepdims=True)
            acc[m] = acc[m] * fade + dot(weights, v_block)
            high[m] = peak

    attend(me)

    def arrive(d):
        p = peer_from(d)
        kv_wait(p)
        kv_forward(p).start()

    def finish(d):
        p = peer_from(d)
        far_wait(p)
        attend(p)

    arrive(1)

    def both(d):
        arrive(d)
        finish(d - 1)

    loop(2, n_sp, both)
    finish(n_sp - 1)

    for h in range(n_head):
        r = slice(h * rows, (h + 1) * rows)
        mixed = acc[0, r, :] / total[0, r, :] - scale_ref[h] * (acc[1, r, :] / total[1, r, :])
        mixed = mixed * lax.rsqrt(jnp.mean(mixed * mixed, axis=-1, keepdims=True) + EPS) * hgain_ref[...]
        heads[:, h * v_cols : (h + 1) * v_cols] = mixed.astype(BF16)

    rows_out = resid_ref.shape[0]
    width = resid_ref.shape[1]
    loads[0].wait()
    block = 512
    for c in range(0, width, block):
        part = dot(heads[...], wout[:, c : c + block]).astype(BF16)
        proj[:, :, c : c + block] = part.reshape(n_tp, rows_out, block)

    def ra_copy(k):
        return copy(proj.at[o_side + 2 * k], ra.at[k], ra_s.at[k], ra_r.at[k], me, partner)

    ra_copy(o_pair).start()
    ra_copy(pair).start()
    ra_copy(o_pair).wait_recv()
    sb[...] = (proj[side + 2 * o_pair].astype(F32) + ra[o_pair].astype(F32)).astype(BF16)
    rb_copy = copy(sb, rb, rb_s, rb_r, me, across)
    rb_copy.start()

    experts = n_sp
    lanes = experts * SUB
    ids = ids_ref[...]
    col = iota((rows_out, lanes), 1)
    hit = [col // SUB == ids[:, j : j + 1] for j in range(2)]
    either = jnp.where(hit[0] | hit[1], 1.0, 0.0).astype(BF16)
    below = jnp.where(
        iota((rows_out, rows_out), 1) < iota((rows_out, rows_out), 0), 1.0, 0.0
    ).astype(BF16)
    slot = dot(below, either).astype(jnp.int32)
    spot = col % SUB
    pieces = SUB // rest
    cut = width // pieces

    def main_table(hits):
        return jnp.where(hits & (slot == spot), 1.0, 0.0).astype(BF16)

    def rest_table(hits, i):
        there = (slot == main + spot % rest) & (spot // rest == i)
        return jnp.where(hits & there, 1.0, 0.0).astype(BF16)

    ra_copy(pair).wait_recv()
    base = resid_ref[...].astype(F32) + (proj[tp].astype(F32) + ra[pair].astype(F32))
    rb_copy.wait_recv()
    now = base + rb[...].astype(F32)
    state[...] = now
    normed = (
        now * lax.rsqrt(jnp.mean(now * now, axis=-1, keepdims=True) + EPS) * ngain_ref[...]
    ).astype(BF16)

    any_hit = hit[0] | hit[1]
    if main:
        om[...] = dot_t(main_table(any_hit), normed).astype(BF16).reshape(om.shape)
    left = jnp.zeros((lanes, cut), F32)
    for i in range(pieces):
        left = left + dot_t(rest_table(any_hit, i), normed[:, i * cut : (i + 1) * cut])
    ol[...] = left.astype(BF16).reshape(ol.shape)

    kinds = ([0] if main else []) + [1]
    out_of, x_of, pr_of, xs_of, xr_of, rs_of, rt_of, y_of = (
        (om, ol), (xm, xl), (prm, prl), (xsm, xsl), (xrm, xrl), (rsm, rsl), (rtm, rtl), (ym, yl)
    )

    def a_send(d, w):
        p = peer_to(d)
        return copy(out_of[w].at[p], x_of[w].at[tp, me], a_s.at[w, p], a_r.at[w, me], p, tp)

    def a_wait(p, w):
        copy(out_of[w].at[p], x_of[w].at[tp, p], a_s.at[w, p], a_r.at[w, p], p, tp).wait_recv()

    def pf(p, w, t):
        spot_ = x_of[w].at[t, p]
        return copy(spot_, spot_, pf_s.at[w, p], pf_r.at[w, p], me, partner)

    def xf(p, w, t):
        spot_ = x_of[w].at[t, p]
        return copy(spot_, spot_, xf_s.at[w, p], xf_r.at[w, p], me, across)

    def rl(p, w, t):
        spot_ = x_of[w].at[t, p]
        return copy(spot_, spot_, rl_s.at[w, p], rl_r.at[w, p], me, partner)

    def for_kinds(fn):
        for w in kinds:
            fn(w)

    loop(1, n_sp, lambda d: for_kinds(lambda w: a_send(d, w).start()))
    for w in kinds:
        x_of[w][tp, me] = out_of[w][me]

    def pass_on(p):
        for w in kinds:
            xf(p, w, tp).start()
            pf(p, w, tp).start()

    pass_on(me)

    def took(d):
        p = peer_from(d)
        for_kinds(lambda w: a_wait(p, w))
        pass_on(p)

    loop(1, n_sp, took)

    near_rows = 2 * n_sp * main
    rest_rows = 2 * n_sp * rest
    all_rows = near_rows + rest_rows
    packed_rows = 2 * n_sp * SUB
    ff = wg.shape[1]

    def packer(i):
        r = iota((rest_rows, packed_rows), 0)
        c = iota((rest_rows, packed_rows), 1)
        there = (r // rest == c // SUB) & (r % rest == c % rest) & ((c % SUB) // rest == i)
        return jnp.where(there, 1.0, 0.0).astype(BF16)

    def serve(which, pr):
        if main:
            xin[:near_rows, :] = xm[pl.ds(2 * pr, 2)].reshape(near_rows, width)
        packed = xl[pl.ds(2 * pr, 2)].reshape(packed_rows, cut)
        for i in range(pieces):
            xin[near_rows:, i * cut : (i + 1) * cut] = dot(packer(i), packed).astype(BF16)
        for c in range(0, ff, 256):
            x = xin[...]
            gate = dot(x, wg[:, c : c + 256])
            up = dot(x, wu[:, c : c + 256])
            hid[:, c : c + 256] = (gate / (1.0 + jnp.exp(-gate)) * up).astype(BF16)
        for c in range(0, width, 256):
            y = dot(hid[...], wd[:, c : c + 256]).astype(BF16)
            if main:
                ym[which, :, :, :, c : c + 256] = y[:near_rows].reshape(2, n_sp, main, 256)
            ytail[:, c : c + 256] = y[near_rows:]
        left_out = jnp.zeros((packed_rows, cut), F32)
        for i in range(pieces):
            left_out = left_out + dot_t(packer(i), ytail[:, i * cut : (i + 1) * cut])
        yl[which] = left_out.astype(BF16).reshape(2, n_sp, SUB, cut)

    def pr_copy(which, w):
        return copy(
            y_of[w].at[which, o_side], pr_of[w].at[which], pr_s.at[w, which], pr_r.at[w, which], me, partner
        )

    loads[1].wait()
    loads[2].wait()
    loads[3].wait()
    loop(0, n_sp, lambda p: for_kinds(lambda w: pf(p, w, partner).wait_recv()))
    serve(0, pair)
    for w in kinds:
        pr_copy(0, w).start()

    def relay(d):
        p = peer_from(d)
        for w in kinds:
            xf(p, w, across).wait_recv()
            rl(p, w, across).start()

    loop(0, n_sp, relay)
    t_far = o_side + 2 * o_pair
    loop(0, n_sp, lambda p: for_kinds(lambda w: rl(p, w, t_far).wait_recv()))
    serve(1, o_pair)
    for w in kinds:
        pr_copy(1, w).start()
    for w in kinds:
        pr_copy(0, w).wait_recv()
        pr_copy(1, w).wait_recv()

    def xs_copy(p, w):
        return copy(xs_of[w].at[p], xr_of[w].at[p], xs_s.at[w, p], xs_r.at[w, p], me, across)

    def send_across(d):
        p = peer_to(d)
        for w in kinds:
            xs_of[w][p] = (y_of[w][1, side, p].astype(F32) + pr_of[w][1, p].astype(F32)).astype(BF16)
            xs_copy(p, w).start()

    loop(1, n_sp + 1, send_across)

    def rt_send(p, w):
        return copy(rs_of[w].at[p], rt_of[w].at[me], rt_s.at[w, p], rt_r.at[w, me], p, tp)

    def summed(p, w):
        near = y_of[w][0, side, p].astype(F32) + pr_of[w][0, p].astype(F32)
        return (near + xr_of[w][p].astype(F32)).astype(BF16)

    def send_back(d):
        p = peer_to(d)
        for w in kinds:
            xs_copy(p, w).wait_recv()
            rs_of[w][p] = summed(p, w)
            rt_send(p, w).start()

    loop(1, n_sp, send_back)
    for w in kinds:
        xs_copy(me, w).wait_recv()
        rt_of[w][me] = summed(me, w)

    def got_back(d):
        p = peer_from(d)
        for w in kinds:
            copy(rs_of[w].at[p], rt_of[w].at[p], rt_s.at[w, p], rt_r.at[w, p], p, tp).wait_recv()

    loop(1, n_sp, got_back)
    weight = rw_ref[...]
    back_left = rtl[...].reshape(lanes, cut)
    for i in range(pieces):
        cols = slice(i * cut, (i + 1) * cut)
        value = state[:, cols]
        for j in range(2):
            picked = dot(rest_table(hit[j], i), back_left)
            if main:
                picked = picked + dot(main_table(hit[j]), rtm[:, :, cols].reshape(lanes, cut))
            value = value + weight[:, j : j + 1] * picked
        out_ref[:, cols] = value.astype(BF16)

    def sent(d):
        p = peer_to(d)
        kv_send(d).wait_send()
        kv_forward(p).wait_send()
        for w in kinds:
            a_send(d, w).wait_send()
            rt_send(p, w).wait_send()

    loop(1, n_sp, sent)

    def sent_all(p):
        for w in kinds:
            pf(p, w, tp).wait_send()
            xf(p, w, tp).wait_send()
            rl(p, w, across).wait_send()
            xs_copy(p, w).wait_send()

    loop(0, n_sp, sent_all)
    ra_copy(0).wait_send()
    ra_copy(1).wait_send()
    rb_copy.wait_send()
    for w in kinds:
        pr_copy(0, w).wait_send()
        pr_copy(1, w).wait_send()


def local(n_sp, n_tp, *args):
    (queries, keys, values, diff_scale, head_gain, w_out, residual, norm_gain, route_ids,
     route_weights, w_gate, w_up, w_down) = args
    rows = queries.shape[0]
    rows_out, width = residual.shape
    top = route_ids.shape[1]
    capacity = max(2, 3 * rows_out * top // (2 * n_sp))
    main = capacity // SUB * SUB
    rest = capacity - main
    cut = width * rest // SUB
    k_cols = keys.shape[1] // KV_HEADS
    v_cols = values.shape[1] // KV_HEADS
    half = k_cols // 2
    n_head = diff_scale.shape[0]
    ff = w_gate.shape[2]
    rest_rows = 2 * n_sp * rest
    all_rows = 2 * n_sp * main + rest_rows

    def bf(*shape):
        return pltpu.VMEM(shape, BF16)

    def two(*lead):
        big = bf(*lead, n_sp, main, width) if main else bf(SUB, 128)
        return [big, bf(*lead, n_sp, SUB, cut)]

    sems = pltpu.SemaphoreType.DMA
    scratch = [
        bf(*w_out.shape), bf(width, ff), bf(width, ff), bf(ff, width),
        bf(n_sp, rows, k_cols + v_cols),
        bf(2, n_head * rows, half),
        pltpu.VMEM((2, n_head * rows, 1), F32),
        pltpu.VMEM((2, n_head * rows, 1), F32),
        pltpu.VMEM((2, n_head * rows, v_cols), F32),
        bf(rows, n_head * v_cols),
        bf(n_tp, rows_out, width),
        bf(2, rows_out, width), bf(rows_out, width), bf(rows_out, width),
        pltpu.VMEM((rows_out, width), F32),
        *two(), *two(n_tp), *two(2, 2), *two(2), *two(), *two(), *two(), *two(),
        bf(all_rows, width), bf(all_rows, ff), bf(rest_rows, width),
        sems((4,)),
        sems((n_sp,)), sems((n_sp,)), sems((n_sp,)), sems((n_sp,)),
        sems((2,)), sems((2,)), sems, sems,
    ]
    for _ in range(4):
        scratch += [sems((2, n_sp)), sems((2, n_sp))]
    scratch += [sems((2, 2)), sems((2, 2))]
    for _ in range(2):
        scratch += [sems((2, n_sp)), sems((2, n_sp))]
    vmem = pl.BlockSpec(memory_space=pltpu.VMEM)
    hbm = pl.BlockSpec(memory_space=pl.ANY)
    smem = pl.BlockSpec(memory_space=pltpu.SMEM)
    return pl.pallas_call(
        functools.partial(kernel, n_sp, n_tp, main, rest),
        out_shape=jax.ShapeDtypeStruct((rows_out, width), BF16),
        in_specs=[vmem, vmem, vmem, smem, vmem, hbm, vmem, vmem, vmem, vmem, hbm, hbm, hbm],
        out_specs=vmem,
        scratch_shapes=scratch,
        compiler_params=pltpu.CompilerParams(
            collective_id=0, has_side_effects=True, vmem_limit_bytes=60 * 1024 * 1024
        ),
    )(
        queries, keys, values, diff_scale, head_gain.reshape(1, -1), w_out, residual,
        norm_gain.reshape(1, -1), route_ids, route_weights, w_gate, w_up, w_down,
    )


def solution(mesh):
    in_specs = (
        P("sp", "tp"),
        P("sp", None),
        P("sp", None),
        P("tp"),
        P(),
        P("tp", None),
        P(("sp", "tp"), None),
        P(),
        P(("sp", "tp"), None),
        P(("sp", "tp"), None),
        P("sp", None, "tp"),
        P("sp", None, "tp"),
        P("sp", "tp", None),
    )
    out_specs = P(("sp", "tp"), None)
    body = functools.partial(local, mesh.shape["sp"], mesh.shape["tp"])
    return jax.shard_map(body, mesh=mesh, in_specs=in_specs, out_specs=out_specs, check_vma=False)
```
